256 devices in a mesh: kv: 16 (over y, x), tp: 16 (over z, core).
Axes of the slice: x: 4, y: 4, z: 8, core: 2. Of those that a mesh axis runs over, the one named last changes fastest.
Arguments:
- tokens: bfloat16 [16, 2048], P(None, 'kv'), may hold values from -40 to 40
- lengths: int32 [16], replicated, may hold values from 1 to 16384, 77824 in all
- cache_keys: bfloat16 [16, 16384, 16, 128], P(None, 'kv', 'tp'), may hold values from -200 to 200
- cache_values: bfloat16 [16, 16384, 16, 128], P(None, 'kv', 'tp'), may hold values from -6 to 6
- lambdas: float32 [16], P('tp'), may hold values from 0.3 to 0.8
- head_gain: bfloat16 [128], replicated, may hold values from 0.099609375 to 1.8984375
- attn_gain: bfloat16 [2048], P('kv'), may hold values from 0.099609375 to 1.8984375
- w_query: bfloat16 [2048, 2048], P('kv', 'tp'), may hold values from -0.125 to 0.125
- w_key: bfloat16 [2048, 2048], P('kv', 'tp'), may hold values from -0.5 to 0.5
- w_value: bfloat16 [2048, 2048], P('kv', 'tp'), may hold values from -0.125 to 0.125
- w_out: bfloat16 [2048, 2048], P('tp', 'kv'), may hold values from -0.125 to 0.125
- first_gain: bfloat16 [2048], P('kv'), may hold values from 0.099609375 to 1.8984375
- first_gate: bfloat16 [2048, 5632], P('kv', 'tp'), may hold values from -0.125 to 0.125
- first_up: bfloat16 [2048, 5632], P('kv', 'tp'), may hold values from -0.125 to 0.125
- first_down: bfloat16 [5632, 2048], P('tp', 'kv'), may hold values from -0.078125 to 0.078125
- second_gain: bfloat16 [2048], P('kv'), may hold values from 0.099609375 to 1.8984375
- second_gate: bfloat16 [2048, 5632], P('kv', 'tp'), may hold values from -0.125 to 0.125
- second_up: bfloat16 [2048, 5632], P('kv', 'tp'), may hold values from -0.125 to 0.125
- second_down: bfloat16 [5632, 2048], P('tp', 'kv'), may hold values from -0.078125 to 0.078125
Outputs:
- stream_out: bfloat16 [16, 2048], P(None, 'kv')
The draws below stay inside these ranges and needn't reach their ends.
Inputs may be any that keep to these rules, and one draw needn't show every extreme that they name: `lengths`: one sequence has exactly 16384 live positions.
All inputs are finite; a program needn't handle non-finite values.
Results may differ from the reference program's by a relative error of at most 0.02.
Values may be sent and summed in bfloat16 or wider, within the bound.
A program may use at most 64 MiB of HBM per device.

```python
import math
import jax
import jax.numpy as jnp
import numpy as np
from jax import lax

D = 2048
FF = 5632
HEADS = 16
DK = 64
DV = 128
SEQS = 16
LENGTH = 16384


def draw_tokens(key, part):
    columns = jnp.arange(D, dtype=jnp.float32) / D
    col_scale = 0.5 * jnp.exp(math.log(4.0) * columns)[None, :]
    base = jnp.clip(jax.random.normal(key, (SEQS, D), jnp.float32), -6.0, 6.0)
    return (base * col_scale).astype(jnp.bfloat16)


def draw_cache_keys(key, part):
    shape_all = (SEQS, LENGTH, HEADS, 2 * DK)
    base = jnp.clip(jax.random.normal(key, shape_all, jnp.float32) * 1.75, -10.0, 10.0)
    return base.astype(jnp.bfloat16)


def steps_of(stream_key, dims, shards, low, largest):
    level = 1.0
    for dim, shards_of in shards:
        draws = jax.random.uniform(jax.random.fold_in(jax.random.fold_in(stream_key, 6), dim), (shards_of,), jnp.float32, low / len(shards), largest / len(shards))
        level = level * jnp.repeat(jnp.exp(draws), dims[dim] // shards_of).reshape((-1,) + (1,) * (len(dims) - 1 - dim))
    return level


def profile(number_of, total, reach, skew):
    portions = [(1 << 20) // math.isqrt(rank ** skew) + 1 for rank in range(2, number_of + 1)]
    surplus, counts = total - reach - (number_of - 1), [1] * (number_of - 1)
    while surplus > 0:
        candidates = [i for i in range(number_of - 1) if counts[i] < reach]
        pool, left = sum([portions[i] for i in candidates]), surplus
        for i in candidates:
            more = min(reach - counts[i], max(1, left * portions[i] // pool), surplus)
            counts[i] = counts[i] + more
            surplus = surplus - more
    return np.array([reach] + counts)


def uneven_parts(own_key, number_of, total, most, slope):
    if number_of == 2:
        one = jax.random.randint(own_key, (), max(1, total - most), min(most, total - 1) + 1)
        return jnp.stack([one, total - one])
    tallies = jnp.asarray(profile(number_of, total, most, slope), jnp.int32)
    pairs = (number_of - 1) // 2
    giver, sink = tallies[1:1 + 2 * pairs:2], tallies[2:2 + 2 * pairs:2]
    slack = jnp.minimum(giver - 1, most - sink)
    moved = jax.random.randint(jax.random.fold_in(own_key, 1), (pairs,), 0, 1 << 20) % (slack + 1)
    tallies = tallies.at[1:1 + 2 * pairs:2].set(giver - moved).at[2:2 + 2 * pairs:2].set(sink + moved)
    return tallies[jax.random.permutation(jax.random.fold_in(own_key, 2), number_of)]


def gaussian(own_key, extent, spread, limit, cuts=(), kind=jnp.bfloat16):
    entries = jax.random.normal(own_key, extent, jnp.float32) * spread
    if len(cuts) > 0:
        entries = steps_of(own_key, extent, cuts, -0.22, 0.18) * entries
    return jnp.clip(entries, min=-limit, max=limit).astype(kind)


def setup_inputs(seed: int = 0) -> dict:
    arg_keys = jax.random.split(jax.random.key(seed), 20)
    tokens = draw_tokens(jax.random.fold_in(arg_keys[19], 71), 0)
    lengths = uneven_parts(arg_keys[1], SEQS, LENGTH + (SEQS - 1) * (LENGTH // 4), LENGTH, 2).astype(jnp.int32)
    cache_keys = draw_cache_keys(jax.random.fold_in(arg_keys[19], 71), 0)
    cache_values = gaussian(arg_keys[3], (SEQS, LENGTH, HEADS, DV), 1.0, 6.0, ((1, 16), (2, 16)))
    lambdas = jnp.clip(0.3 + 0.5 * jax.random.uniform(arg_keys[4], (HEADS,), jnp.float32) ** steps_of(arg_keys[4], (HEADS,), ((0, 16),), -0.2, 0.2), 0.3, 0.8)
    head_gain = jnp.clip(1.0 + 0.18 * jax.random.normal(arg_keys[5], (DV,), jnp.float32), 0.099609375, 1.8984375).astype(jnp.bfloat16)
    attn_gain = jnp.clip(1.0 + 0.18 * jax.random.normal(arg_keys[6], (D,), jnp.float32), 0.099609375, 1.8984375).astype(jnp.bfloat16)
    w_query = gaussian(arg_keys[7], (D, HEADS * 2 * DK), D ** -0.5, 0.125, ((0, 16), (1, 16)))
    w_key = gaussian(arg_keys[8], (D, HEADS * 2 * DK), (D // 16) ** -0.5, 0.5, ((0, 16), (1, 16)))
    w_value = gaussian(arg_keys[9], (D, HEADS * DV), D ** -0.5, 0.125, ((0, 16), (1, 16)))
    w_out = gaussian(arg_keys[10], (HEADS * DV, D), (HEADS * DV) ** -0.5, 0.125, ((0, 16), (1, 16)))
    first_gain = jnp.clip(1.0 + 0.18 * jax.random.normal(arg_keys[11], (D,), jnp.float32), 0.099609375, 1.8984375).astype(jnp.bfloat16)
    first_gate = gaussian(arg_keys[12], (D, FF), D ** -0.5, 0.125, ((0, 16), (1, 16)))
    first_up = gaussian(arg_keys[13], (D, FF), D ** -0.5, 0.125, ((0, 16), (1, 16)))
    first_down = gaussian(arg_keys[14], (FF, D), FF ** -0.5, 0.078125, ((0, 16), (1, 16)))
    second_gain = jnp.clip(1.0 + 0.18 * jax.random.normal(arg_keys[15], (D,), jnp.float32), 0.099609375, 1.8984375).astype(jnp.bfloat16)
    second_gate = gaussian(arg_keys[16], (D, FF), D ** -0.5, 0.125, ((0, 16), (1, 16)))
    second_up = gaussian(arg_keys[17], (D, FF), D ** -0.5, 0.125, ((0, 16), (1, 16)))
    second_down = gaussian(arg_keys[18], (FF, D), FF ** -0.5, 0.078125, ((0, 16), (1, 16)))
    return {"tokens": tokens, "lengths": lengths, "cache_keys": cache_keys, "cache_values": cache_values, "lambdas": lambdas, "head_gain": head_gain, "attn_gain": attn_gain, "w_query": w_query, "w_key": w_key, "w_value": w_value, "w_out": w_out, "first_gain": first_gain, "first_gate": first_gate, "first_up": first_up, "first_down": first_down, "second_gain": second_gain, "second_gate": second_gate, "second_up": second_up, "second_down": second_down}


EPSILON = 1e-06
ROTARY_BASE = 10000.0
OUTPUT_KEEP = 0.8

def rotate(vectors, positions):
    half_width = vectors.shape[-1] // 2
    inv_freq = jnp.power(ROTARY_BASE, -jnp.arange(half_width, dtype=jnp.float32) / half_width)
    angles = positions.astype(jnp.float32)[:, None] * inv_freq[None, :]
    bcast_shape = (angles.shape[0],) + (1,) * (vectors.ndim - 2) + (half_width,)
    cosine = jnp.cos(angles).reshape(bcast_shape)
    sine_part = jnp.sin(angles).reshape(bcast_shape)
    first_half = vectors[..., :half_width]
    second_half = vectors[..., half_width:]
    return jnp.concatenate([first_half * cosine - second_half * sine_part, second_half * cosine + first_half * sine_part], axis=-1)

def channel_mix(stream, gain, w_gate, w_up, w_down):
    stream_f = stream.astype(jnp.float32)
    scaled = (stream_f * gain.astype(jnp.float32)).astype(jnp.bfloat16)
    row_scale = lax.rsqrt(lax.optimization_barrier(jnp.mean(stream_f * stream_f, axis=1, keepdims=True)) + EPSILON)
    gate = row_scale * jnp.dot(scaled, w_gate, preferred_element_type=jnp.float32)
    up_val = row_scale * jnp.dot(scaled, w_up, preferred_element_type=jnp.float32)
    hidden = (jax.nn.silu(gate) * up_val).astype(jnp.bfloat16)
    return (stream_f + 0.5 * jnp.dot(hidden, w_down, preferred_element_type=jnp.float32)).astype(jnp.bfloat16)

def reference(tokens, lengths, cache_keys, cache_values, lambdas, head_gain, attn_gain, w_query, w_key, w_value, w_out, first_gain, first_gate, first_up, first_down, second_gain, second_gate, second_up, second_down):
    first = channel_mix(tokens, first_gain, first_gate, first_up, first_down)
    seq_count = first.shape[0]
    stream_f = first.astype(jnp.float32)
    scaled = (stream_f * attn_gain.astype(jnp.float32)).astype(jnp.bfloat16)
    row_scale = lax.rsqrt(lax.optimization_barrier(jnp.mean(stream_f * stream_f, axis=1, keepdims=True)) + EPSILON)
    query = row_scale * jnp.dot(scaled, w_query, preferred_element_type=jnp.float32)
    key_new = row_scale * jnp.dot(scaled, w_key, preferred_element_type=jnp.float32)
    value_new = (row_scale * jnp.dot(scaled, w_value, preferred_element_type=jnp.float32)).astype(jnp.bfloat16)
    query = rotate(query.reshape(seq_count, HEADS, 2, DK), lengths).astype(jnp.bfloat16)
    key_new = rotate(key_new.reshape(seq_count, HEADS, 2, DK), lengths).astype(jnp.bfloat16)
    value_new = value_new.reshape(seq_count, HEADS, DV)
    live_mask = jnp.arange(LENGTH, dtype=jnp.int32)[None, :] < lengths[:, None]
    scale_att = DK ** (-0.5)

    def one_head(inputs):
        index, lam_value = inputs
        key_rows = lax.dynamic_index_in_dim(cache_keys, index, axis=2, keepdims=False).reshape(seq_count, LENGTH, 2, DK).astype(jnp.float32)
        value_rows = lax.dynamic_index_in_dim(cache_values, index, axis=2, keepdims=False).astype(jnp.float32)
        query_h = lax.dynamic_index_in_dim(query, index, axis=1, keepdims=False).astype(jnp.float32)
        key_h = lax.dynamic_index_in_dim(key_new, index, axis=1, keepdims=False).astype(jnp.float32)
        value_h = lax.dynamic_index_in_dim(value_new, index, axis=1, keepdims=False).astype(jnp.float32)
        scores = jnp.einsum('bcd,blcd->bcl', query_h, key_rows, precision=lax.Precision.HIGHEST) * scale_att
        scores = jnp.where(live_mask[:, None, :], scores, -jnp.inf)
        own_score = lax.optimization_barrier(jnp.sum(query_h * key_h, axis=2)) * scale_att
        peak_max = jnp.maximum(lax.optimization_barrier(jnp.max(scores, axis=2)), own_score)
        weights = jnp.exp(scores - peak_max[..., None])
        fresh_weight = jnp.exp(own_score - peak_max)
        denominator = lax.optimization_barrier(jnp.sum(weights, axis=2)) + fresh_weight
        rounded = lax.optimization_barrier(weights.astype(jnp.bfloat16)).astype(jnp.float32)
        summed = jnp.einsum('bcl,bld->bcd', rounded, value_rows, precision=lax.Precision.HIGHEST) + fresh_weight[..., None] * value_h[:, None, :]
        mixed = summed / denominator[..., None]
        return mixed[:, 0] - lam_value * mixed[:, 1]
    heads_out = lax.map(one_head, (jnp.arange(HEADS, dtype=jnp.int32), lambdas))
    heads_out = jnp.moveaxis(heads_out, 0, 1)
    norm_scale = lax.rsqrt(lax.optimization_barrier(jnp.mean(heads_out * heads_out, axis=2, keepdims=True)) + EPSILON)
    normed = (heads_out * norm_scale * head_gain.astype(jnp.float32) * OUTPUT_KEEP).astype(jnp.bfloat16)
    normed = normed.reshape(seq_count, HEADS * DV)
    second = (stream_f + jnp.dot(normed, w_out, preferred_element_type=jnp.float32)).astype(jnp.bfloat16)
    return channel_mix(second, second_gain, second_gate, second_up, second_down)
```

```python
import functools

import jax
import jax.numpy as jnp
import numpy as np
from jax import lax
from jax.experimental import pallas as pl
from jax.experimental.pallas import tpu as pltpu
from jax.sharding import PartitionSpec as P

MESH = pl.DeviceIdType.MESH
F32 = jnp.float32
BF16 = jnp.bfloat16

D = 2048
DK = 64
DV = 128
SIDE = 4
DEEP = 8
GROUP = 16
SEQS = 16
BLOCK = 1024
UNITS = 352
WIDE = 384

EPSILON = 1e-06
ROTARY_BASE = 10000.0
OUTPUT_KEEP = 0.8
MASKED_SCORE = -1e30
NT = (((1,), (1,)), ((), ()))


def lane_of(shape):
    return lax.broadcasted_iota(jnp.int32, shape, len(shape) - 1)


def row_of(shape):
    return lax.broadcasted_iota(jnp.int32, shape, len(shape) - 2)


def rounded(value):
    return value.astype(BF16).astype(F32)


def added(buf):
    total = buf[0].astype(F32)
    for i in range(1, GROUP):
        total = total + buf[i].astype(F32)
    return total


def kernel(
    lengths,
    lambdas,
    inv_freq,
    tokens,
    keys,
    values,
    head_gain,
    attn_gain,
    w_query,
    w_key,
    w_value,
    w_out,
    first_gain,
    first_gate,
    first_up,
    first_down,
    second_gain,
    second_gate,
    second_up,
    second_down,
    out,
    v_tokens,
    v_freq,
    v_gains,
    v_wide,
    v_down,
    v_qkv,
    v_out,
    v_keys,
    v_values,
    b_mix1,
    b_down1,
    b_qkv,
    b_attn,
    b_proj,
    b_mix2,
    b_down2,
    local_sem,
    send_sem,
    recv_sem,
):
    kv, tp = lax.axis_index("kv"), lax.axis_index("tp")
    y, x = kv // SIDE, kv % SIDE
    z, core = tp // 2, tp % 2

    started = []

    def fetch(src, dst):
        copy = pltpu.make_async_copy(src, dst, local_sem.at[len(started)])
        copy.start()
        started.append(copy)
        return copy

    c_tokens = fetch(tokens, v_tokens)
    c_gain1 = fetch(first_gain, v_gains.at[0])
    c_gate1 = fetch(first_gate, v_wide.at[0, pl.ds(0, UNITS)])
    c_up1 = fetch(first_up, v_wide.at[0, pl.ds(WIDE, UNITS)])
    c_down1 = fetch(first_down, v_down.at[0, pl.ds(0, UNITS)])
    c_freq = fetch(inv_freq, v_freq)
    c_gain2 = fetch(attn_gain, v_gains.at[1])
    c_q = fetch(w_query, v_qkv.at[:, pl.ds(0, 128)])
    c_k = fetch(w_key, v_qkv.at[:, pl.ds(128, 128)])
    c_v = fetch(w_value, v_qkv.at[:, pl.ds(256, 128)])
    c_keys = fetch(keys, v_keys)
    c_values = fetch(values, v_values)
    c_gain3 = fetch(head_gain, v_gains.at[2])
    c_out = fetch(w_out, v_out)
    c_gain4 = fetch(second_gain, v_gains.at[3])
    c_gate2 = fetch(second_gate, v_wide.at[1, pl.ds(0, UNITS)])
    c_up2 = fetch(second_up, v_wide.at[1, pl.ds(WIDE, UNITS)])
    c_down2 = fetch(second_down, v_down.at[1, pl.ds(0, UNITS)])

    reach = lambda step, side: min(step, side - step)
    plane = sorted(
        ((dy, dx) for dy in range(SIDE) for dx in range(SIDE) if dy or dx),
        key=lambda s: -reach(s[0], SIDE) - reach(s[1], SIDE),
    )
    column = sorted(
        ((dz, dc) for dz in range(DEEP) for dc in range(2) if dz or dc),
        key=lambda s: -2 * reach(s[0], DEEP) - s[1],
    )
    kv_peers = [(((y + dy) % SIDE) * SIDE + (x + dx) % SIDE, tp) for dy, dx in plane]
    tp_peers = [(kv, ((z + dz) % DEEP) * 2 + (core + dc) % 2) for dz, dc in column]

    barrier = pltpu.get_barrier_semaphore()
    for peer in kv_peers + tp_peers:
        pl.semaphore_signal(barrier, inc=1, device_id=peer, device_id_type=MESH)

    def send(phase, buf, me, peers):
        for peer in peers:
            pltpu.make_async_remote_copy(
                src_ref=buf.at[me],
                dst_ref=buf.at[me],
                send_sem=send_sem.at[phase],
                recv_sem=recv_sem.at[phase],
                device_id=peer,
                device_id_type=MESH,
            ).start()

    def settle(buf, sem):
        others = buf.at[pl.ds(0, GROUP - 1)]
        pltpu.make_async_copy(others, others, sem).wait()

    for half in range(2):
        for at in (UNITS, WIDE + UNITS):
            v_wide[half, pl.ds(at, WIDE - UNITS)] = jnp.zeros((WIDE - UNITS, 128), BF16)
        v_down[half, pl.ds(UNITS, WIDE - UNITS)] = jnp.zeros((WIDE - UNITS, 128), BF16)

    def gain_row(at):
        return v_gains[at].astype(F32)

    wide_lane = lane_of((SEQS, 2 * WIDE))
    tile_lane = lane_of((SEQS, 128))
    SQ = UNITS - 256

    def mix_partial(stream, gain, at, buf):
        scaled = (stream * gain).astype(BF16)
        part = lax.dot_general(scaled, v_wide[at], NT, preferred_element_type=F32)
        square = jnp.sum(stream * stream, axis=1, keepdims=True)
        high = rounded(square)
        part = jnp.where(wide_lane == UNITS, high, part)
        part = jnp.where(wide_lane == UNITS + 1, square - high, part)
        buf[kv] = part.astype(BF16)

    def mix_hidden(buf):
        total = added(buf)
        third = total[:, 256:384]
        own = (tile_lane == SQ) | (tile_lane == SQ + 1)
        square = jnp.sum(jnp.where(own, third, 0.0), axis=1, keepdims=True)
        scale = lax.rsqrt(square / D + EPSILON)
        gate, up = scale * total[:, :WIDE], scale * total[:, WIDE:]
        return (jax.nn.silu(gate) * up).astype(BF16)

    c_tokens.wait()
    c_gain1.wait()
    c_gate1.wait()
    c_up1.wait()
    stream = v_tokens[...].astype(F32)
    mix_partial(stream, gain_row(0), 0, b_mix1)
    pl.semaphore_wait(barrier, 2 * (GROUP - 1))
    send(0, b_mix1, kv, kv_peers)

    c_freq.wait()
    small = (SEQS, 128)
    row = row_of(small)
    lens = jnp.zeros(small, jnp.int32)
    for b in range(SEQS):
        lens = jnp.where(row == b, lengths[b], lens)
    angles = lens.astype(F32) * v_freq[...]
    cosine, sine = jnp.cos(angles), jnp.sin(angles)
    in_half = tile_lane % DK < DK // 2
    sine = jnp.where(in_half, -sine, sine)
    c_down1.wait()
    for copy in (c_gain2, c_q, c_k, c_v):
        copy.wait()

    settle(b_mix1, recv_sem.at[0])
    hidden = mix_hidden(b_mix1)
    b_down1[tp] = jnp.dot(hidden, v_down[0], preferred_element_type=F32).astype(BF16)
    send(1, b_down1, tp, tp_peers)
    for copy in (c_keys, c_values, c_gain3, c_out, c_gain4, c_gate2, c_up2, c_down2):
        copy.wait()
    settle(b_down1, recv_sem.at[1])
    first = rounded(stream + 0.5 * added(b_down1))

    scaled = (first * gain_row(1)).astype(BF16)
    part = jnp.dot(scaled, v_qkv[...], preferred_element_type=F32)
    square = jnp.sum(first * first, axis=1, keepdims=True)
    lane8 = lane_of((8, 128))
    high = rounded(square)
    low = square - high
    stats = jnp.zeros((8, 128), F32)
    for at, column_of in enumerate((high[:8], high[8:], low[:8], low[8:])):
        stats = jnp.where(lane8 == at, column_of, stats)
    for at in range(3):
        b_qkv[kv, pl.ds(at * SEQS, SEQS)] = part[:, at * 128 : (at + 1) * 128].astype(BF16)
    b_qkv[kv, pl.ds(3 * SEQS, 8)] = stats.astype(BF16)
    send(2, b_qkv, kv, kv_peers)
    settle(b_qkv, recv_sem.at[2])
    total = added(b_qkv)
    stats = total[3 * SEQS :]
    squares = [
        jnp.sum(jnp.where((lane8 == at) | (lane8 == at + 2), stats, 0.0), axis=1, keepdims=True)
        for at in range(2)
    ]
    scale = lax.rsqrt(jnp.concatenate(squares, axis=0) / D + EPSILON)

    def rotate(vectors):
        swapped = jnp.where(in_half, pltpu.roll(vectors, 96, 1), pltpu.roll(vectors, 32, 1))
        return rounded(vectors * cosine + swapped * sine)

    query = rotate(scale * total[:SEQS])
    key_new = rotate(scale * total[SEQS : 2 * SEQS])
    value_new = rounded(scale * total[2 * SEQS : 3 * SEQS])

    scale_att = DK ** (-0.5)
    front = tile_lane < DK
    both = jnp.concatenate([jnp.where(front, query, 0.0), jnp.where(front, 0.0, query)], axis=0)
    row2 = row_of((2 * SEQS, 128)) % SEQS
    scores = jnp.zeros((2 * SEQS, BLOCK), F32)
    for pair in range(SEQS // 2):
        b = 2 * pair
        lhs = jnp.concatenate(
            [jnp.where(row2 == b + k, both, 0.0).astype(BF16) for k in range(2)], axis=1
        )
        rhs = jnp.concatenate([v_keys[b + k] for k in range(2)], axis=1)
        scores = scores + lax.dot_general(lhs, rhs, NT, preferred_element_type=F32)
    lens2 = jnp.concatenate([lens, lens], axis=0)
    lens_wide = jnp.concatenate([lens2] * (BLOCK // 128), axis=1)
    live = kv * BLOCK + lane_of((2 * SEQS, BLOCK)) < lens_wide
    scores = jnp.where(live, scores * scale_att, MASKED_SCORE)
    block_max = jnp.max(scores, axis=1, keepdims=True)
    weights = jnp.where(live, jnp.exp(scores - block_max), 0.0)
    block_sum = jnp.sum(weights, axis=1, keepdims=True)
    weights = weights.astype(BF16)
    mixed = jnp.zeros((2 * SEQS, DV), F32)
    for pair in range(SEQS // 2):
        b = 2 * pair
        rhs = jnp.concatenate([v_values[b + k] for k in range(2)], axis=1)
        product = jnp.dot(weights, rhs, preferred_element_type=F32)
        for k in range(2):
            mixed = jnp.where(row2 == b + k, product[:, k * DV : (k + 1) * DV], mixed)
    b_attn[kv, pl.ds(0, 2 * SEQS)] = mixed.astype(BF16)

    def packed(columns):
        tile = jnp.zeros((8, 128), F32)
        for at, column_of in enumerate(columns):
            tile = jnp.where(lane8 == at, column_of, tile)
        return tile

    quarters = [slice(8 * k, 8 * k + 8) for k in range(4)]
    peak = packed([block_max[q] for q in quarters])
    weight = packed([block_sum[q] for q in quarters])
    peak_high = rounded(peak)
    peak_mid = rounded(peak - peak_high)
    weight_high = rounded(weight)
    stats = peak_high + pltpu.roll(peak_mid, 4, 1) + pltpu.roll(peak - peak_high - peak_mid, 8, 1)
    stats = stats + pltpu.roll(weight_high, 12, 1) + pltpu.roll(weight - weight_high, 16, 1)
    b_attn[kv, pl.ds(2 * SEQS, 8)] = stats.astype(BF16)
    send(3, b_attn, kv, kv_peers)

    product = query * key_new * scale_att
    own = [jnp.sum(jnp.where(f, product, 0.0), axis=1, keepdims=True) for f in (front, ~front)]
    own_score = packed([own[k // 2][8 * (k % 2) : 8 * (k % 2) + 8] for k in range(4)])

    settle(b_attn, recv_sem.at[3])
    peaks, sums = [], []
    for i in range(GROUP):
        tile = b_attn[i, pl.ds(2 * SEQS, 8)].astype(F32)
        peaks.append(tile + pltpu.roll(tile, 124, 1) + pltpu.roll(tile, 120, 1))
        sums.append(pltpu.roll(tile, 116, 1) + pltpu.roll(tile, 112, 1))
    peak = functools.reduce(jnp.maximum, peaks, own_score)
    shares = [jnp.exp(p - peak) for p in peaks]
    fresh = jnp.exp(own_score - peak)
    total_sum = fresh
    for share, s in zip(shares, sums):
        total_sum = total_sum + share * s
    inverse = 1.0 / total_sum
    fresh = fresh * inverse
    shares = [share * inverse for share in shares]
    rows = []
    for k in range(4):
        half = 8 * (k % 2)
        acc = fresh[:, k : k + 1] * value_new[half : half + 8]
        for i in range(GROUP):
            acc = acc + shares[i][:, k : k + 1] * b_attn[i, pl.ds(8 * k, 8)].astype(F32)
        rows.append(acc)
    heads = jnp.concatenate(rows[:2], axis=0) - lambdas[0] * jnp.concatenate(rows[2:], axis=0)
    spread = jnp.sum(heads * heads, axis=1, keepdims=True) / DV
    normed = heads * lax.rsqrt(spread + EPSILON) * gain_row(2) * OUTPUT_KEEP
    b_proj[tp] = jnp.dot(normed.astype(BF16), v_out[...], preferred_element_type=F32).astype(BF16)
    send(4, b_proj, tp, tp_peers)
    settle(b_proj, recv_sem.at[4])
    second = rounded(first + added(b_proj))

    mix_partial(second, gain_row(3), 1, b_mix2)
    send(5, b_mix2, kv, kv_peers)
    settle(b_mix2, recv_sem.at[5])
    hidden = mix_hidden(b_mix2)
    b_down2[tp] = jnp.dot(hidden, v_down[1], preferred_element_type=F32).astype(BF16)
    send(6, b_down2, tp, tp_peers)
    settle(b_down2, recv_sem.at[6])
    out[...] = (second + 0.5 * added(b_down2)).astype(BF16)

    for phase, buf in enumerate((b_mix1, b_down1, b_qkv, b_attn, b_proj, b_mix2, b_down2)):
        settle(buf, send_sem.at[phase])


def local(
    tokens,
    lengths,
    cache_keys,
    cache_values,
    lambdas,
    head_gain,
    attn_gain,
    w_query,
    w_key,
    w_value,
    w_out,
    first_gain,
    first_gate,
    first_up,
    first_down,
    second_gain,
    second_gate,
    second_up,
    second_down,
):
    inv_freq = (ROTARY_BASE ** (-(np.arange(128) % 32) / 32.0)).astype(np.float32)
    flat = (SEQS, BLOCK, DV)
    operands = (
        lengths,
        lambdas,
        jnp.asarray(inv_freq).reshape(1, 128),
        tokens,
        cache_keys.reshape(flat),
        cache_values.reshape(flat),
        head_gain.reshape(1, 128),
        attn_gain.reshape(1, 128),
        w_query,
        w_key,
        w_value,
        w_out,
        first_gain.reshape(1, 128),
        first_gate.T,
        first_up.T,
        first_down,
        second_gain.reshape(1, 128),
        second_gate.T,
        second_up.T,
        second_down,
    )
    smem = pl.BlockSpec(memory_space=pltpu.SMEM)
    hbm = pl.BlockSpec(memory_space=pltpu.HBM)
    return pl.pallas_call(
        kernel,
        name="layer",
        out_shape=jax.ShapeDtypeStruct((SEQS, 128), BF16),
        in_specs=[smem, smem] + [hbm] * (len(operands) - 2),
        out_specs=pl.BlockSpec(memory_space=pltpu.VMEM),
        scratch_shapes=[
            pltpu.VMEM((SEQS, 128), BF16),
            pltpu.VMEM((1, 128), F32),
            pltpu.VMEM((4, 1, 128), BF16),
            pltpu.VMEM((2, 2 * WIDE, 128), BF16),
            pltpu.VMEM((2, WIDE, 128), BF16),
            pltpu.VMEM((128, 384), BF16),
            pltpu.VMEM((128, 128), BF16),
            pltpu.VMEM(flat, BF16),
            pltpu.VMEM(flat, BF16),
            pltpu.VMEM((GROUP, SEQS, 2 * WIDE), BF16),
            pltpu.VMEM((GROUP, SEQS, 128), BF16),
            pltpu.VMEM((GROUP, 3 * SEQS + 8, 128), BF16),
            pltpu.VMEM((GROUP, 2 * SEQS + 8, 128), BF16),
            pltpu.VMEM((GROUP, SEQS, 128), BF16),
            pltpu.VMEM((GROUP, SEQS, 2 * WIDE), BF16),
            pltpu.VMEM((GROUP, SEQS, 128), BF16),
            pltpu.SemaphoreType.DMA((18,)),
            pltpu.SemaphoreType.DMA((7,)),
            pltpu.SemaphoreType.DMA((7,)),
        ],
        compiler_params=pltpu.CompilerParams(
            collective_id=0, has_side_effects=True, vmem_limit_bytes=67_043_328
        ),
    )(*operands)


def solution(mesh):
    placed = (
        P(None, "kv"),
        P(),
        P(None, "kv", "tp", None),
        P(None, "kv", "tp", None),
        P("tp"),
        P(),
        P("kv"),
        P("kv", "tp"),
        P("kv", "tp"),
        P("kv", "tp"),
        P("tp", "kv"),
        P("kv"),
        P("kv", "tp"),
        P("kv", "tp"),
        P("tp", "kv"),
        P("kv"),
        P("kv", "tp"),
        P("kv", "tp"),
        P("tp", "kv"),
    )
    return jax.shard_map(
        local, mesh=mesh, in_specs=placed, out_specs=P(None, "kv"), check_vma=False
    )
```

```python
import functools

import jax
import jax.numpy as jnp
import numpy as np
from jax import lax
from jax.experimental import pallas as pl
from jax.experimental.pallas import tpu as pltpu
from jax.sharding import PartitionSpec as P

MESH = pl.DeviceIdType.MESH
F32 = jnp.float32
BF16 = jnp.bfloat16

D = 2048
DK = 64
DV = 128
SIDE = 4
DEEP = 8
GROUP = 16
SEQS = 16
BLOCK = 1024
UNITS = 352
WIDE = 384

EPSILON = 1e-06
ROTARY_BASE = 10000.0
OUTPUT_KEEP = 0.8
MASKED_SCORE = -1e30
NT = (((1,), (1,)), ((), ()))


def lane_of(shape):
    return lax.broadcasted_iota(jnp.int32, shape, len(shape) - 1)


def row_of(shape):
    return lax.broadcasted_iota(jnp.int32, shape, len(shape) - 2)


def rounded(value):
    return value.astype(BF16).astype(F32)


def added(buf):
    total = buf[0].astype(F32)
    for i in range(1, GROUP):
        total = total + buf[i].astype(F32)
    return total


def kernel(
    lengths,
    lambdas,
    inv_freq,
    tokens,
    keys,
    values,
    head_gain,
    attn_gain,
    w_query,
    w_key,
    w_value,
    w_out,
    first_gain,
    first_gate,
    first_up,
    first_down,
    second_gain,
    second_gate,
    second_up,
    second_down,
    out,
    v_tokens,
    v_freq,
    v_gains,
    v_wide,
    v_down,
    v_qkv,
    v_out,
    v_keys,
    v_values,
    v_keys_t,
    v_result,
    s_lengths,
    b_mix1,
    b_down1,
    b_query,
    b_fresh,
    b_attn,
    b_proj,
    b_mix2,
    b_down2,
    local_sem,
    send_sem,
    recv_sem,
):
    kv, tp = lax.axis_index("kv"), lax.axis_index("tp")
    y, x = kv // SIDE, kv % SIDE
    z, core = tp // 2, tp % 2

    reach = lambda step, side: min(step, side - step)
    plane = sorted(
        ((dy, dx) for dy in range(SIDE) for dx in range(SIDE) if dy or dx),
        key=lambda s: -reach(s[0], SIDE) - reach(s[1], SIDE),
    )
    column = sorted(
        ((dz, dc) for dz in range(DEEP) for dc in range(2) if dz or dc),
        key=lambda s: -2 * reach(s[0], DEEP) - s[1],
    )
    kv_peers = [(((y + dy) % SIDE) * SIDE + (x + dx) % SIDE, tp) for dy, dx in plane]
    tp_peers = [(kv, ((z + dz) % DEEP) * 2 + (core + dc) % 2) for dz, dc in column]

    barrier = pltpu.get_barrier_semaphore()
    for peer in kv_peers + tp_peers:
        pl.semaphore_signal(barrier, inc=1, device_id=peer, device_id_type=MESH)

    started = []

    def fetch(src, dst):
        copy = pltpu.make_async_copy(src, dst, local_sem.at[len(started)])
        copy.start()
        started.append(copy)
        return copy

    c_tokens = fetch(tokens, v_tokens)
    c_gain1 = fetch(first_gain, v_gains.at[0])
    c_gate1 = fetch(first_gate, v_wide.at[0, pl.ds(0, UNITS)])
    c_up1 = fetch(first_up, v_wide.at[0, pl.ds(WIDE, UNITS)])
    c_lengths = fetch(lengths, s_lengths)
    c_keys = fetch(keys, v_keys)
    c_down1 = fetch(first_down, v_down.at[0, pl.ds(0, UNITS)])
    c_freq = fetch(inv_freq, v_freq)
    c_gain2 = fetch(attn_gain, v_gains.at[1])
    c_q = fetch(w_query, v_qkv.at[:, pl.ds(0, 128)])
    c_k = fetch(w_key, v_qkv.at[:, pl.ds(128, 128)])
    c_v = fetch(w_value, v_qkv.at[:, pl.ds(256, 128)])
    c_values = fetch(values, v_values)
    c_gain3 = fetch(head_gain, v_gains.at[2])
    c_out = fetch(w_out, v_out)
    c_gain4 = fetch(second_gain, v_gains.at[3])
    c_gate2 = fetch(second_gate, v_wide.at[1, pl.ds(0, UNITS)])
    c_up2 = fetch(second_up, v_wide.at[1, pl.ds(WIDE, UNITS)])
    c_down2 = fetch(second_down, v_down.at[1, pl.ds(0, UNITS)])

    def send(phase, buf, me, peers):
        for peer in peers:
            pltpu.make_async_remote_copy(
                src_ref=buf.at[me],
                dst_ref=buf.at[me],
                send_sem=send_sem.at[phase],
                recv_sem=recv_sem.at[phase],
                device_id=peer,
                device_id_type=MESH,
            ).start()

    def settle(buf, sem):
        others = buf.at[pl.ds(0, GROUP - 1)]
        pltpu.make_async_copy(others, others, sem).wait()

    for half in range(2):
        for at in (UNITS, WIDE + UNITS):
            v_wide[half, pl.ds(at, WIDE - UNITS)] = jnp.zeros((WIDE - UNITS, 128), BF16)
        v_down[half, pl.ds(UNITS, WIDE - UNITS)] = jnp.zeros((WIDE - UNITS, 128), BF16)

    def gain_row(at):
        return v_gains[at].astype(F32)

    wide_lane = lane_of((SEQS, 2 * WIDE))
    tile_lane = lane_of((SEQS, 128))
    SQ = UNITS - 256

    def mix_partial(stream, gain, at, buf):
        scaled = (stream * gain).astype(BF16)
        part = lax.dot_general(scaled, v_wide[at], NT, preferred_element_type=F32)
        square = jnp.sum(stream * stream, axis=1, keepdims=True)
        high = rounded(square)
        part = jnp.where(wide_lane == UNITS, high, part)
        part = jnp.where(wide_lane == UNITS + 1, square - high, part)
        buf[kv] = part.astype(BF16)

    def mix_hidden(buf):
        total = added(buf)
        third = total[:, 256:384]
        own = (tile_lane == SQ) | (tile_lane == SQ + 1)
        square = jnp.sum(jnp.where(own, third, 0.0), axis=1, keepdims=True)
        scale = lax.rsqrt(square / D + EPSILON)
        gate, up = scale * total[:, :WIDE], scale * total[:, WIDE:]
        return (jax.nn.silu(gate) * up).astype(BF16)

    c_tokens.wait()
    c_gain1.wait()
    c_gate1.wait()
    c_up1.wait()
    stream = v_tokens[...].astype(F32)
    mix_partial(stream, gain_row(0), 0, b_mix1)
    pl.semaphore_wait(barrier, 2 * (GROUP - 1))
    send(0, b_mix1, kv, kv_peers)

    c_freq.wait()
    c_lengths.wait()
    small = (SEQS, 128)
    row = row_of(small)
    lens = jnp.zeros(small, jnp.int32)
    for b in range(SEQS):
        lens = jnp.where(row == b, s_lengths[b], lens)
    angles = lens.astype(F32) * v_freq[...]
    cosine, sine = jnp.cos(angles), jnp.sin(angles)
    in_half = tile_lane % DK < DK // 2
    sine = jnp.where(in_half, -sine, sine)
    c_keys.wait()

    def turn(b, carry):
        v_keys_t[pl.ds(pl.multiple_of(b * 128, 128), 128)] = v_keys[b].T
        return carry

    lax.fori_loop(0, SEQS, turn, 0)
    c_down1.wait()
    for copy in (c_gain2, c_q, c_k, c_v):
        copy.wait()

    settle(b_mix1, recv_sem.at[0])
    hidden = mix_hidden(b_mix1)
    b_down1[tp] = jnp.dot(hidden, v_down[0], preferred_element_type=F32).astype(BF16)
    send(1, b_down1, tp, tp_peers)
    for copy in (c_values, c_gain3, c_out, c_gain4, c_gate2, c_up2, c_down2):
        copy.wait()
    settle(b_down1, recv_sem.at[1])
    first = rounded(stream + 0.5 * added(b_down1))

    scaled = (first * gain_row(1)).astype(BF16)
    part = jnp.dot(scaled, v_qkv[...], preferred_element_type=F32)
    square = jnp.sum(first * first, axis=1, keepdims=True)
    lane8 = lane_of((8, 128))
    high = rounded(square)
    low = square - high
    stats = jnp.zeros((8, 128), F32)
    for at, column_of in enumerate((high[:8], high[8:], low[:8], low[8:])):
        stats = jnp.where(lane8 == at, column_of, stats)
    b_query[kv, pl.ds(0, SEQS)] = part[:, :128].astype(BF16)
    b_query[kv, pl.ds(SEQS, 8)] = stats.astype(BF16)
    send(2, b_query, kv, kv_peers)
    b_fresh[kv, pl.ds(0, SEQS)] = part[:, 128:256].astype(BF16)
    b_fresh[kv, pl.ds(SEQS, SEQS)] = part[:, 256:].astype(BF16)
    send(3, b_fresh, kv, kv_peers)
    settle(b_query, recv_sem.at[2])
    total = added(b_query)
    stats = total[SEQS:]
    squares = [
        jnp.sum(jnp.where((lane8 == at) | (lane8 == at + 2), stats, 0.0), axis=1, keepdims=True)
        for at in range(2)
    ]
    scale = lax.rsqrt(jnp.concatenate(squares, axis=0) / D + EPSILON)

    def rotate(vectors):
        swapped = jnp.where(in_half, pltpu.roll(vectors, 96, 1), pltpu.roll(vectors, 32, 1))
        return rounded(vectors * cosine + swapped * sine)

    query = rotate(scale * total[:SEQS])

    scale_att = DK ** (-0.5)
    front = tile_lane < DK
    rows8 = row_of(small) % 8
    live_lane = kv * BLOCK + lane_of((SEQS, BLOCK))
    peaks, sums = [], []
    for g in range(2):
        mine = query[8 * g : 8 * g + 8]
        twice = jnp.concatenate([mine, mine], axis=0)
        both = jnp.where((row < 8) == front, twice, 0.0)
        lhs = jnp.concatenate([jnp.where(rows8 == b, both, 0.0).astype(BF16) for b in range(8)], axis=1)
        scores = jnp.dot(lhs, v_keys_t[pl.ds(g * BLOCK, BLOCK)], preferred_element_type=F32)
        lens_g = lens[8 * g : 8 * g + 8]
        lens_g = jnp.concatenate([lens_g, lens_g], axis=0)
        live = live_lane < jnp.concatenate([lens_g] * (BLOCK // 128), axis=1)
        scores = jnp.where(live, scores * scale_att, MASKED_SCORE)
        block_max = jnp.max(scores, axis=1, keepdims=True)
        weights = jnp.where(live, jnp.exp(scores - block_max), 0.0)
        sums.append(jnp.sum(weights, axis=1, keepdims=True))
        peaks.append(block_max)
        weights = weights.astype(BF16)
        mixed = jnp.zeros(small, F32)
        for pair in range(4):
            b = 8 * g + 2 * pair
            rhs = jnp.concatenate([v_values[b + k] for k in range(2)], axis=1)
            product = jnp.dot(weights, rhs, preferred_element_type=F32)
            for k in range(2):
                mixed = jnp.where(rows8 == 2 * pair + k, product[:, k * DV : (k + 1) * DV], mixed)
        b_attn[kv, pl.ds(SEQS * g, SEQS)] = mixed.astype(BF16)

    wide = (2 * SEQS, 128)
    diagonal = lane_of(wide) % 32 == row_of(wide)

    def laid(columns):
        return jnp.sum(jnp.where(diagonal, jnp.concatenate(columns, axis=0), 0.0), axis=0, keepdims=True)

    peak, weight = laid(peaks), laid(sums)
    peak_high = rounded(peak)
    peak_mid = rounded(peak - peak_high)
    weight_high = rounded(weight)
    tile = jnp.zeros((8, 128), F32)
    row8 = row_of((8, 128))
    terms = (peak_high, peak_mid, peak - peak_high - peak_mid, weight_high, weight - weight_high)
    for at, term in enumerate(terms):
        tile = jnp.where(row8 == at, term, tile)
    b_attn[kv, pl.ds(2 * SEQS, 8)] = tile.astype(BF16)
    send(4, b_attn, kv, kv_peers)

    settle(b_fresh, recv_sem.at[3])
    total = added(b_fresh)
    key_new = rotate(scale * total[:SEQS])
    value_new = scale * total[SEQS:]
    product = query * key_new * scale_att
    own = [jnp.sum(jnp.where(f, product, 0.0), axis=1, keepdims=True) for f in (front, ~front)]
    own_score = laid([own[k % 2][8 * (k // 2) : 8 * (k // 2) + 8] for k in range(4)])
    fresh_rows = [value_new[8 * (k // 2) : 8 * (k // 2) + 8] for k in range(4)]
    fresh_rows = jnp.concatenate(fresh_rows + [jnp.zeros((96, 128), F32)], axis=0).astype(BF16)

    settle(b_attn, recv_sem.at[4])
    part_of = lane_of((8, 128)) // 32
    block_peaks, block_sums = [], []
    for q in range(4):
        tile = b_attn[4 * q, pl.ds(2 * SEQS, 8)].astype(F32)
        for k in range(1, 4):
            tile = jnp.where(part_of == k, b_attn[4 * q + k, pl.ds(2 * SEQS, 8)].astype(F32), tile)
        block_peaks.append(tile[0:1] + tile[1:2] + tile[2:3])
        block_sums.append(tile[3:4] + tile[4:5])

    def around(value, combine):
        return functools.reduce(combine, [pltpu.roll(value, 32 * k, 1) for k in range(1, 4)], value)

    peak = jnp.maximum(around(functools.reduce(jnp.maximum, block_peaks), jnp.maximum), own_score)
    shares = [jnp.exp(p - peak) for p in block_peaks]
    fresh = jnp.exp(own_score - peak)
    weighted = [share * s for share, s in zip(shares, block_sums)]
    inverse = 1.0 / (around(functools.reduce(jnp.add, weighted), jnp.add) + fresh)
    factors = [jnp.where(diagonal, share * inverse, 0.0) for share in shares]
    factors.append(jnp.where(lane_of(wide) == row_of(wide), fresh * inverse, 0.0))
    factors = jnp.concatenate(factors, axis=1)
    high = factors.astype(BF16)
    low = (factors - high.astype(F32)).astype(BF16)
    blocks = [b_attn[i, pl.ds(0, 2 * SEQS)] for i in range(GROUP)]
    blocks = jnp.concatenate(blocks + [fresh_rows], axis=0)
    mixed = jnp.dot(jnp.concatenate([high, low], axis=0), blocks, preferred_element_type=F32)
    mixed = mixed[: 2 * SEQS] + mixed[2 * SEQS :]
    heads = [mixed[16 * g : 16 * g + 8] - lambdas[0] * mixed[16 * g + 8 : 16 * g + 16] for g in range(2)]
    heads = jnp.concatenate(heads, axis=0)
    spread = jnp.sum(heads * heads, axis=1, keepdims=True) / DV
    normed = heads * lax.rsqrt(spread + EPSILON) * gain_row(2) * OUTPUT_KEEP
    b_proj[tp] = jnp.dot(normed.astype(BF16), v_out[...], preferred_element_type=F32).astype(BF16)
    send(5, b_proj, tp, tp_peers)
    settle(b_proj, recv_sem.at[5])
    second = rounded(first + added(b_proj))

    mix_partial(second, gain_row(3), 1, b_mix2)
    send(6, b_mix2, kv, kv_peers)
    settle(b_mix2, recv_sem.at[6])
    hidden = mix_hidden(b_mix2)
    b_down2[tp] = jnp.dot(hidden, v_down[1], preferred_element_type=F32).astype(BF16)
    send(7, b_down2, tp, tp_peers)
    settle(b_down2, recv_sem.at[7])
    v_result[...] = (second + 0.5 * added(b_down2)).astype(BF16)

    finished = fetch(v_result, out)
    sent = (b_mix1, b_down1, b_query, b_fresh, b_attn, b_proj, b_mix2, b_down2)
    for phase, buf in enumerate(sent):
        settle(buf, send_sem.at[phase])
    finished.wait()


def local(
    tokens,
    lengths,
    cache_keys,
    cache_values,
    lambdas,
    head_gain,
    attn_gain,
    w_query,
    w_key,
    w_value,
    w_out,
    first_gain,
    first_gate,
    first_up,
    first_down,
    second_gain,
    second_gate,
    second_up,
    second_down,
):
    inv_freq = (ROTARY_BASE ** (-(np.arange(128) % 32) / 32.0)).astype(np.float32)
    flat = (SEQS, BLOCK, DV)
    operands = (
        lengths,
        lambdas,
        jnp.asarray(inv_freq).reshape(1, 128),
        tokens,
        cache_keys.reshape(flat),
        cache_values.reshape(flat),
        head_gain.reshape(1, 128),
        attn_gain.reshape(1, 128),
        w_query,
        w_key,
        w_value,
        w_out,
        first_gain.reshape(1, 128),
        first_gate.T,
        first_up.T,
        first_down,
        second_gain.reshape(1, 128),
        second_gate.T,
        second_up.T,
        second_down,
    )
    hbm = pl.BlockSpec(memory_space=pltpu.HBM)
    return pl.pallas_call(
        kernel,
        name="layer",
        out_shape=jax.ShapeDtypeStruct((SEQS, 128), BF16),
        in_specs=[hbm, pl.BlockSpec(memory_space=pltpu.SMEM)] + [hbm] * (len(operands) - 2),
        out_specs=hbm,
        scratch_shapes=[
            pltpu.VMEM((SEQS, 128), BF16),
            pltpu.VMEM((1, 128), F32),
            pltpu.VMEM((4, 1, 128), BF16),
            pltpu.VMEM((2, 2 * WIDE, 128), BF16),
            pltpu.VMEM((2, WIDE, 128), BF16),
            pltpu.VMEM((128, 384), BF16),
            pltpu.VMEM((128, 128), BF16),
            pltpu.VMEM(flat, BF16),
            pltpu.VMEM(flat, BF16),
            pltpu.VMEM((SEQS * 128, BLOCK), BF16),
            pltpu.VMEM((SEQS, 128), BF16),
            pltpu.SMEM((SEQS,), jnp.int32),
            pltpu.VMEM((GROUP, SEQS, 2 * WIDE), BF16),
            pltpu.VMEM((GROUP, SEQS, 128), BF16),
            pltpu.VMEM((GROUP, SEQS + 8, 128), BF16),
            pltpu.VMEM((GROUP, 2 * SEQS, 128), BF16),
            pltpu.VMEM((GROUP, 2 * SEQS + 8, 128), BF16),
            pltpu.VMEM((GROUP, SEQS, 128), BF16),
            pltpu.VMEM((GROUP, SEQS, 2 * WIDE), BF16),
            pltpu.VMEM((GROUP, SEQS, 128), BF16),
            pltpu.SemaphoreType.DMA((20,)),
            pltpu.SemaphoreType.DMA((8,)),
            pltpu.SemaphoreType.DMA((8,)),
        ],
        compiler_params=pltpu.CompilerParams(
            collective_id=0, has_side_effects=True, vmem_limit_bytes=67_043_328
        ),
    )(*operands)


def solution(mesh):
    placed = (
        P(None, "kv"),
        P(),
        P(None, "kv", "tp", None),
        P(None, "kv", "tp", None),
        P("tp"),
        P(),
        P("kv"),
        P("kv", "tp"),
        P("kv", "tp"),
        P("kv", "tp"),
        P("tp", "kv"),
        P("kv"),
        P("kv", "tp"),
        P("kv", "tp"),
        P("tp", "kv"),
        P("kv"),
        P("kv", "tp"),
        P("kv", "tp"),
        P("tp", "kv"),
    )
    return jax.shard_map(
        local, mesh=mesh, in_specs=placed, out_specs=P(None, "kv"), check_vma=False
    )
```
